32 devices in a mesh: kv: 8 (over z, x), tp: 4 (over y, core).
Axes of the slice: x: 2, y: 2, z: 4, core: 2. Of those that a mesh axis runs over, the one named last changes fastest.
Arguments:
- tokens: bfloat16 [1024, 2048], P('kv'), may hold values from -64 to 64
- query_weight: bfloat16 [2048, 1024], P(None, 'tp'), may hold values from -0.125 to 0.125
- key_weight: bfloat16 [2048, 256], P(None, 'tp'), may hold values from -0.125 to 0.125
- value_weight: bfloat16 [2048, 256], P(None, 'tp'), may hold values from -0.125 to 0.125
- out_weight: bfloat16 [1024, 2048], P(None, 'tp'), may hold values from -0.1875 to 0.1875
- alibi_slope: float32 [16], P('tp'), may hold values from 0.00024414062 to 0.03
- block_choice: int32 [32, 8], P('kv'), may hold values from -1 to 31, as said below
Outputs:
- mixed: bfloat16 [1024, 2048], P('kv', 'tp')
The draws below stay inside these ranges and needn't reach their ends.
Inputs may be any that keep to these rules, and one draw needn't show every extreme that they name: `block_choice`: row g begins with g; its other entries are distinct blocks below g, or -1 where nothing is chosen. The rows of one index of kv (aligned runs of 4 rows) together name at most one block of any other index of kv, and some rows of each index name a block of the index before it and of the index half the axis before it where those exist.
All inputs are finite; a program needn't handle non-finite values.
Results may differ from the reference program's by a relative error of at most 0.012.
Values may be sent and summed in bfloat16 or wider, within the bound.
A program may use at most 64 MiB of HBM per device.

```python
import math
import jax
import jax.numpy as jnp
from jax import lax

D = 2048
HEADS = 16
KV_HEADS = 4
HEAD = 64
BLOCK = 32
TOPK = 8
BLK_DEV = 4
NBLK = 32
TOKENS = 1024
ATTN = 1024


def draw_tokens(key, part):
    first, second = jax.random.split(key)
    values = jax.random.normal(first, (TOKENS, D), jnp.float32)
    return jnp.clip(values, -64.0, 64.0).astype(jnp.bfloat16)


def draw_block_choice(key, part):
    processor_roster = NBLK // BLK_DEV
    first, second, third = jax.random.split(key, 3)
    pick_table = jax.random.randint(first, (processor_roster, processor_roster), 0, BLK_DEV)
    favoured_tiles = (jax.random.randint(second, (processor_roster,), 0, 4) == 0).astype(jnp.int32) * 16384
    stochastic_jitter = jax.random.randint(third, (NBLK, NBLK), 0, 16384)
    rows = jnp.arange(NBLK, dtype=jnp.int32)[:, None]
    cols = jnp.arange(NBLK, dtype=jnp.int32)[None, :]
    down_shard_number = rows // BLK_DEV
    across_shard_number = cols // BLK_DEV
    local = down_shard_number == across_shard_number
    remote_fit = cols % BLK_DEV == pick_table[down_shard_number, across_shard_number]
    usable = (cols < rows) & (local | remote_fit)
    rating_increment = jnp.where((across_shard_number == down_shard_number - 1) | (across_shard_number == down_shard_number - processor_roster // 2), 32768, 0)
    tile_rating = stochastic_jitter + favoured_tiles[across_shard_number] + rating_increment
    combined = jnp.where(usable, tile_rating * 16384 + cols, -1)
    best, _ = lax.top_k(combined, TOPK - 1)
    others = jnp.where(best >= 0, best % 16384, -1)
    return jnp.concatenate([rows, others], axis=1).astype(jnp.int32)


def block_scale(rng, dims, shards, least, high):
    def one(dim, blocks):
        draws = jax.random.uniform(jax.random.fold_in(jax.random.fold_in(rng, 6), dim), (blocks,), jnp.float32, least / len(shards), high / len(shards))
        return jnp.repeat(jnp.exp(draws), dims[dim] // blocks).reshape((-1,) + (1,) * (len(dims) - dim - 1))

    level = one(*shards[0])
    for cut in shards[1:]:
        level = level * one(*cut)
    return level


def normal_values(rng, shape, scale, bound, pieces=(), kind=jnp.bfloat16):
    array = scale * jax.random.normal(rng, shape, jnp.float32)
    if pieces:
        array = array * block_scale(rng, shape, pieces, -0.22, 0.18)
    return jnp.clip(array, -bound, bound).astype(kind)


def setup_inputs(seed: int = 0) -> dict:
    arg_keys = jax.random.split(jax.random.key(seed), 8)
    tokens = draw_tokens(jax.random.fold_in(arg_keys[7], 71), 0)
    query_weight = normal_values(arg_keys[1], (D, ATTN), D ** -0.5, 0.125, ((1, 4),))
    key_weight = normal_values(arg_keys[2], (D, KV_HEADS * HEAD), D ** -0.5, 0.125, ((1, 4),))
    value_weight = normal_values(arg_keys[3], (D, KV_HEADS * HEAD), D ** -0.5, 0.125, ((1, 4),))
    out_weight = normal_values(arg_keys[4], (ATTN, D), ATTN ** -0.5, 0.1875, ((1, 4),))
    alibi_slope = jnp.clip(jnp.exp(math.log(0.03) - 4.8112082 * jax.random.uniform(arg_keys[5], (HEADS,), jnp.float32) ** block_scale(arg_keys[5], (HEADS,), ((0, 4),), -0.2, 0.2)), 0.00024414062, 0.03)
    block_choice = draw_block_choice(jax.random.fold_in(arg_keys[7], 71), 0)
    return {"tokens": tokens, "query_weight": query_weight, "key_weight": key_weight, "value_weight": value_weight, "out_weight": out_weight, "alibi_slope": alibi_slope, "block_choice": block_choice}


def reference(tokens, query_weight, key_weight, value_weight, out_weight, alibi_slope, block_choice):
    queries = jnp.dot(tokens, query_weight, preferred_element_type=jnp.float32).astype(jnp.bfloat16)
    keys = jnp.dot(tokens, key_weight, preferred_element_type=jnp.float32).astype(jnp.bfloat16)
    values = jnp.dot(tokens, value_weight, preferred_element_type=jnp.float32).astype(jnp.bfloat16)
    group = HEADS // KV_HEADS
    query_blocks = queries.reshape(NBLK, BLOCK, HEADS, HEAD)
    key_blocks = keys.reshape(NBLK, BLOCK, KV_HEADS, HEAD)
    value_blocks = values.reshape(NBLK, BLOCK, KV_HEADS, HEAD)
    scale = HEAD ** -0.5

    def one_block(args):
        block_id, query_blk, chosen = args
        safe_ids = jnp.maximum(chosen, 0)
        picked_keys = jnp.repeat(key_blocks[safe_ids], group, axis=2).astype(jnp.float32)
        picked_values = jnp.repeat(value_blocks[safe_ids], group, axis=2).astype(jnp.float32)
        scores = jnp.einsum('qhd,nkhd->hqnk', query_blk.astype(jnp.float32), picked_keys) * scale
        query_pos = block_id * BLOCK + jnp.arange(BLOCK, dtype=jnp.int32)
        key_pos = safe_ids[:, None] * BLOCK + jnp.arange(BLOCK, dtype=jnp.int32)[None, :]
        distance = query_pos[:, None, None] - key_pos[None, :, :]
        scores = scores - alibi_slope[:, None, None, None] * distance.astype(jnp.float32)[None]
        keep = (chosen >= 0)[None, :, None] & (distance >= 0)
        scores = jnp.where(keep[None], scores, -jnp.inf)
        weights = jax.nn.softmax(scores, axis=(2, 3)).astype(jnp.bfloat16)
        attended = jnp.einsum('hqnk,nkhd->qhd', weights.astype(jnp.float32), picked_values)
        return attended.astype(jnp.bfloat16).reshape(BLOCK, HEADS * HEAD)

    attended = lax.map(one_block, (jnp.arange(NBLK, dtype=jnp.int32), query_blocks, block_choice))
    attended = attended.reshape(TOKENS, HEADS * HEAD)
    return jnp.dot(attended, out_weight, preferred_element_type=jnp.float32).astype(jnp.bfloat16)
```

```python
import functools

import jax
import jax.numpy as jnp
from jax import lax
from jax.experimental import pallas as pl
from jax.experimental.pallas import tpu as pltpu
from jax.sharding import PartitionSpec as P

HEAD = 64
BLOCK = 32
LANES = 2 * HEAD
FULL_FROM = 64
NEVER = 1 << 28


def each(low, high, body):
    if high - low <= 16:
        for i in range(low, high):
            body(i)
    else:
        pl.loop(low, high)(body)


def kernel(n_kv, n_tp, tok_hbm, wq_hbm, wk_hbm, wv_hbm, wo_hbm, slope, choice, choice_vec,
           out, tok, wq, wkv, wo, table, want_out, want_in, send_buf, q_pad, bias, att,
           load_sem, want_send, want_recv, kv_send, kv_recv, att_send, att_recv):
    me = lax.axis_index("kv")
    mt = lax.axis_index("tp")
    rows = tok.shape[0]
    nb = rows // BLOCK
    heads = wq.shape[1] // HEAD
    topk = choice.shape[1]
    picked = topk * BLOCK
    stacked = heads * BLOCK

    loads = [
        pltpu.make_async_copy(tok_hbm, tok, load_sem.at[0]),
        pltpu.make_async_copy(wk_hbm, wkv.at[pl.ds(0, HEAD)], load_sem.at[1]),
        pltpu.make_async_copy(wv_hbm, wkv.at[pl.ds(HEAD, HEAD)], load_sem.at[2]),
        pltpu.make_async_copy(wq_hbm, wq, load_sem.at[3]),
        pltpu.make_async_copy(wo_hbm, wo, load_sem.at[4]),
    ]
    barrier = pltpu.get_barrier_semaphore()
    each(1, n_kv, lambda k: pl.semaphore_signal(
        barrier, inc=1, device_id={"kv": lax.rem(me + k, n_kv)}))
    for d in range(1, n_tp):
        pl.semaphore_signal(barrier, inc=1, device_id={"tp": lax.rem(mt + d, n_tp)})
    for load in loads:
        load.start()

    ids = choice_vec[...]
    owner = ids // nb
    local = ids - owner * nb

    def note_want(k):
        hit = (ids >= 0) & (owner == me - k)
        found = jnp.max(jnp.where(hit, local, -1).astype(jnp.float32), keepdims=True)
        want_out[k] = jnp.broadcast_to(found, (8, LANES))

    each(1, min(n_kv, FULL_FROM) if n_kv <= 16 else n_kv, note_want)

    for load in loads[:3]:
        load.wait()
    kv = lax.dot_general(tok[...], wkv[...], (((1,), (1,)), ((), ())),
                         preferred_element_type=jnp.float32).astype(jnp.bfloat16)
    table[pl.ds(0, nb)] = kv.reshape(nb, BLOCK, LANES)

    pl.semaphore_wait(barrier, n_kv - 1 + n_tp - 1)

    def wanted_only(k):
        return n_kv > 16 or k < FULL_FROM

    def want_copy(k):
        return pltpu.make_async_remote_copy(
            src_ref=want_out.at[k], dst_ref=want_in.at[k],
            send_sem=want_send.at[k], recv_sem=want_recv.at[k],
            device_id={"kv": lax.rem(me - k + n_kv, n_kv)})

    def kv_copy(k):
        whole = not wanted_only(k)
        return pltpu.make_async_remote_copy(
            src_ref=table.at[pl.ds(0, nb)] if whole else send_buf.at[k],
            dst_ref=table.at[pl.ds(k * nb, nb)] if whole else table.at[k * nb],
            send_sem=kv_send.at[k], recv_sem=kv_recv.at[k],
            device_id={"kv": lax.rem(me + k, n_kv)})

    def first_sends(k):
        if wanted_only(k):
            @pl.when(me - k >= 0)
            def _():
                want_copy(k).start()
        else:
            @pl.when(me + k < n_kv)
            def _():
                kv_copy(k).start()

    if n_kv <= 16:
        for k in reversed(range(1, n_kv)):
            first_sends(k)
    else:
        each(1, n_kv, first_sends)

    lane = lax.broadcasted_iota(jnp.int32, (1, LANES), 1)
    low = lane < HEAD
    loads[3].wait()
    queries = jnp.dot(tok[...], wq[...], preferred_element_type=jnp.float32)
    queries = queries * (HEAD ** -0.5)
    for pair in range(heads // 2):
        two = queries[:, pair * LANES:(pair + 1) * LANES]
        swapped = pltpu.roll(two, HEAD, 1)
        for half, part in enumerate((two, swapped)):
            part = jnp.where(low, part, 0.0).astype(jnp.bfloat16)
            head = 2 * pair + half
            for g in range(nb):
                q_pad[g, head * BLOCK:(head + 1) * BLOCK, :] = part[g * BLOCK:(g + 1) * BLOCK]

    def answer(k):
        if wanted_only(k):
            @pl.when(me + k < n_kv)
            def _():
                want_copy(k).wait_recv()
                want = want_in[k]
                chosen = jnp.zeros((BLOCK // 8, 8, LANES), jnp.float32)
                for b in range(nb):
                    blk = table[b].astype(jnp.float32).reshape(BLOCK // 8, 8, LANES)
                    chosen = jnp.where((want == float(b))[None], blk, chosen)
                send_buf[k] = chosen.reshape(BLOCK, LANES).astype(jnp.bfloat16)
                kv_copy(k).start()

    each(1, n_kv, answer)

    row = lax.broadcasted_iota(jnp.int32, (stacked, 1), 0)
    slope_col = jnp.zeros((stacked, 1), jnp.float32)
    for h in range(heads):
        slope_col = jnp.where(row // BLOCK == h, slope[h], slope_col)
    q_in = lax.rem(row, BLOCK)
    col = lax.broadcasted_iota(jnp.int32, (1, picked), 1)
    rows_of = []
    for g in range(nb):
        base = jnp.zeros((1, picked), jnp.int32)
        here = []
        for j in range(topk):
            c = choice[g, j]
            base = jnp.where(col // BLOCK == j, jnp.where(c < 0, NEVER, c * BLOCK), base)
            safe = jnp.where(c < 0, me * nb, c)
            own = safe // nb
            k = me - own
            loc = safe - own * nb
            exact = k == 0
            if n_kv <= 16:
                exact = exact | (k >= FULL_FROM)
            here.append(k * nb + jnp.where(exact, loc, 0))
        rows_of.append(here)
        key_pos = base + lax.rem(col, BLOCK)
        dist = ((me * nb + g) * BLOCK + q_in) - key_pos
        bias[g] = jnp.where(dist >= 0, -slope_col * dist.astype(jnp.float32), -jnp.inf)

    def kv_arrived(k):
        @pl.when(me - k >= 0)
        def _():
            kv_copy(k).wait_recv()

    each(1, n_kv, kv_arrived)

    keep_hi = jnp.where(low, 0.0, 1.0).astype(jnp.bfloat16)
    ones_lo = jnp.where(low, 1.0, 0.0).astype(jnp.bfloat16)

    partner = mt + 1 - 2 * lax.rem(mt, 2)
    peers = [partner]
    for i in range(2, n_tp, 2):
        peers += [lax.rem(mt + i, n_tp), lax.rem(partner + i, n_tp)]

    def att_copy(p, g, source):
        piece = att.at[source, pl.ds(g * BLOCK, BLOCK)]
        return pltpu.make_async_remote_copy(
            src_ref=piece, dst_ref=piece,
            send_sem=att_send.at[p, g], recv_sem=att_recv.at[source, g],
            device_id={"tp": peers[p]})

    for g in range(nb):
        chosen = jnp.concatenate([table[r] for r in rows_of[g]], axis=0)
        scores = lax.dot_general(q_pad[g], chosen, (((1,), (1,)), ((), ())),
                                 preferred_element_type=jnp.float32) + bias[g]
        top = jnp.max(scores, axis=1, keepdims=True)
        weights = jnp.exp(scores - top).astype(jnp.bfloat16)
        got = jnp.dot(weights, chosen * keep_hi + ones_lo, preferred_element_type=jnp.float32)
        turned = pltpu.roll(got, HEAD, 1)
        for pair in range(heads // 2):
            even = slice(2 * pair * BLOCK, (2 * pair + 1) * BLOCK)
            odd = slice((2 * pair + 1) * BLOCK, (2 * pair + 2) * BLOCK)
            num = jnp.where(low, turned[even], got[odd])
            den = jnp.where(low, got[even], turned[odd])
            att[mt, pl.ds(g * BLOCK, BLOCK), pl.ds(pair * LANES, LANES)] = (num / den).astype(jnp.bfloat16)
        for p in reversed(range(n_tp - 1)):
            att_copy(p, g, mt).start()

    width = heads * HEAD

    def term(source):
        return jnp.dot(att[source], wo[pl.ds(source * width, width)],
                       preferred_element_type=jnp.float32)

    loads[4].wait()
    total = term(mt)
    for p in range(n_tp - 1):
        for g in range(nb):
            att_copy(p, g, peers[p]).wait_recv()
        total += term(peers[p])
    out[...] = total.astype(out.dtype)

    def finish(k):
        if wanted_only(k):
            @pl.when(me - k >= 0)
            def _():
                want_copy(k).wait_send()

        @pl.when(me + k < n_kv)
        def _():
            kv_copy(k).wait_send()

    each(1, n_kv, finish)
    for p in range(n_tp - 1):
        for g in range(nb):
            att_copy(p, g, mt).wait_send()


def shards(n_kv, n_tp, tokens, query_weight, key_weight, value_weight, out_weight, alibi_slope, block_choice):
    rows, depth = tokens.shape
    nb = rows // BLOCK
    width = query_weight.shape[1]
    heads = width // HEAD
    topk = block_choice.shape[1]
    hbm = pl.BlockSpec(memory_space=pltpu.HBM)
    smem = pl.BlockSpec(memory_space=pltpu.SMEM)
    vmem = pl.BlockSpec(memory_space=pltpu.VMEM)
    bf16 = jnp.bfloat16
    dma = pltpu.SemaphoreType.DMA
    return pl.pallas_call(
        functools.partial(kernel, n_kv, n_tp),
        out_shape=jax.ShapeDtypeStruct((rows, out_weight.shape[1]), bf16),
        in_specs=[hbm] * 5 + [smem, smem, vmem],
        out_specs=vmem,
        scratch_shapes=[
            pltpu.VMEM((rows, depth), bf16),
            pltpu.VMEM((depth, width), bf16),
            pltpu.VMEM((LANES, depth), bf16),
            pltpu.VMEM(out_weight.shape, bf16),
            pltpu.VMEM((n_kv * nb, BLOCK, LANES), bf16),
            pltpu.VMEM((n_kv, 8, LANES), jnp.float32),
            pltpu.VMEM((n_kv, 8, LANES), jnp.float32),
            pltpu.VMEM((n_kv, BLOCK, LANES), bf16),
            pltpu.VMEM((nb, heads * BLOCK, LANES), bf16),
            pltpu.VMEM((nb, heads * BLOCK, topk * BLOCK), jnp.float32),
            pltpu.VMEM((n_tp, rows, width), bf16),
            dma((5,)),
            dma((n_kv,)),
            dma((n_kv,)),
            dma((n_kv,)),
            dma((n_kv,)),
            dma((n_tp - 1, nb)),
            dma((n_tp, nb)),
        ],
        compiler_params=pltpu.CompilerParams(collective_id=0, has_side_effects=True),
    )(tokens, query_weight, key_weight.T, value_weight.T, out_weight, alibi_slope, block_choice, block_choice)


def solution(mesh):
    in_specs = (
        P("kv", None),
        P(None, "tp"),
        P(None, "tp"),
        P(None, "tp"),
        P(None, "tp"),
        P("tp"),
        P("kv", None),
    )
    body = functools.partial(shards, mesh.shape["kv"], mesh.shape["tp"])
    return jax.shard_map(body, mesh=mesh, in_specs=in_specs, out_specs=P("kv", "tp"), check_vma=False)
```

```python
import functools

import jax
import jax.numpy as jnp
from jax import lax
from jax.experimental import pallas as pl
from jax.experimental.pallas import tpu as pltpu
from jax.sharding import PartitionSpec as P

HEAD = 64
BLOCK = 32
LANES = 2 * HEAD
FULL_FROM = 64
NEVER = 1 << 28
GROUP = 2


def each(low, high, body):
    if high - low <= 16:
        for i in range(low, high):
            body(i)
    else:
        pl.loop(low, high)(body)


def kernel(n_kv, n_tp, tok_hbm, wq_hbm, wk_hbm, wv_hbm, wo_hbm, slope_hbm, choice_hbm,
           out, slope, choice, choice_vec, tok, wq, wkv, wo, table, want_out, want_in, send_buf, q_pad, bias, att,
           load_sem, want_send, want_recv, kv_send, kv_recv, att_send, att_recv):
    me = lax.axis_index("kv")
    mt = lax.axis_index("tp")
    rows = tok.shape[0]
    nb = rows // BLOCK
    heads = wq.shape[1] // HEAD
    topk = choice.shape[1]
    picked = topk * BLOCK
    stacked = heads * BLOCK

    loads = [
        pltpu.make_async_copy(tok_hbm, tok, load_sem.at[0]),
        pltpu.make_async_copy(wk_hbm, wkv.at[pl.ds(0, HEAD)], load_sem.at[1]),
        pltpu.make_async_copy(wv_hbm, wkv.at[pl.ds(HEAD, HEAD)], load_sem.at[2]),
        pltpu.make_async_copy(wq_hbm, wq, load_sem.at[3]),
        pltpu.make_async_copy(wo_hbm, wo, load_sem.at[4]),
    ]
    small = [
        pltpu.make_async_copy(choice_hbm, choice_vec, load_sem.at[5]),
        pltpu.make_async_copy(choice_hbm, choice, load_sem.at[6]),
        pltpu.make_async_copy(slope_hbm, slope, load_sem.at[7]),
    ]
    barrier = pltpu.get_barrier_semaphore()
    each(1, n_kv, lambda k: pl.semaphore_signal(
        barrier, inc=1, device_id={"kv": lax.rem(me + k, n_kv)}))
    for d in range(1, n_tp):
        pl.semaphore_signal(barrier, inc=1, device_id={"tp": lax.rem(mt + d, n_tp)})
    for load in small + loads:
        load.start()

    small[0].wait()
    ids = choice_vec[...]
    owner = ids // nb
    local = ids - owner * nb

    def note_want(k):
        hit = (ids >= 0) & (owner == me - k)
        found = jnp.max(jnp.where(hit, local, -1).astype(jnp.float32), keepdims=True)
        want_out[k] = jnp.broadcast_to(found, (8, LANES))

    each(1, min(n_kv, FULL_FROM) if n_kv <= 16 else n_kv, note_want)

    def wanted_only(k):
        return n_kv > 16 or k < FULL_FROM

    def want_copy(k):
        return pltpu.make_async_remote_copy(
            src_ref=want_out.at[k], dst_ref=want_in.at[k],
            send_sem=want_send.at[k], recv_sem=want_recv.at[k],
            device_id={"kv": lax.rem(me - k + n_kv, n_kv)})

    def kv_copy(k):
        whole = not wanted_only(k)
        return pltpu.make_async_remote_copy(
            src_ref=table.at[pl.ds(0, nb)] if whole else send_buf.at[k],
            dst_ref=table.at[pl.ds(k * nb, nb)] if whole else table.at[k * nb],
            send_sem=kv_send.at[k], recv_sem=kv_recv.at[k],
            device_id={"kv": lax.rem(me + k, n_kv)})

    def ask(k):
        if wanted_only(k):
            @pl.when(me - k >= 0)
            def _():
                want_copy(k).start()

    def meet():
        pl.semaphore_wait(barrier, n_kv - 1 + n_tp - 1)
        each(1, n_kv, ask)

    early = me * 2 >= n_kv
    pl.when(early)(meet)

    for load in loads[:3]:
        load.wait()
    kv = lax.dot_general(tok[...], wkv[...], (((1,), (1,)), ((), ())),
                         preferred_element_type=jnp.float32).astype(jnp.bfloat16)
    table[pl.ds(0, nb)] = kv.reshape(nb, BLOCK, LANES)

    lane = lax.broadcasted_iota(jnp.int32, (1, LANES), 1)
    low = lane < HEAD
    loads[3].wait()
    queries = jnp.dot(tok[...], wq[...], preferred_element_type=jnp.float32)
    queries = queries * (HEAD ** -0.5)
    for pair in range(heads // 2):
        two = queries[:, pair * LANES:(pair + 1) * LANES]
        swapped = pltpu.roll(two, HEAD, 1)
        for half, part in enumerate((two, swapped)):
            part = jnp.where(low, part, 0.0).astype(jnp.bfloat16)
            head = 2 * pair + half
            for g in range(nb):
                q_pad[g, head * BLOCK:(head + 1) * BLOCK, :] = part[g * BLOCK:(g + 1) * BLOCK]

    def answer(k):
        if wanted_only(k):
            @pl.when(me + k < n_kv)
            def _():
                want_copy(k).wait_recv()
                want = want_in[k]
                chosen = jnp.zeros((BLOCK // 8, 8, LANES), jnp.float32)
                for b in range(nb):
                    blk = table[b].astype(jnp.float32).reshape(BLOCK // 8, 8, LANES)
                    chosen = jnp.where((want == float(b))[None], blk, chosen)
                send_buf[k] = chosen.reshape(BLOCK, LANES).astype(jnp.bfloat16)
                kv_copy(k).start()

    pl.when(jnp.logical_not(early))(meet)

    def send_all(k):
        if not wanted_only(k):
            @pl.when(me + k < n_kv)
            def _():
                kv_copy(k).start()

    each(1, n_kv, send_all)
    each(1, n_kv, answer)

    small[1].wait()
    small[2].wait()
    row = lax.broadcasted_iota(jnp.int32, (stacked, 1), 0)
    slope_col = jnp.zeros((stacked, 1), jnp.float32)
    for h in range(heads):
        slope_col = jnp.where(row // BLOCK == h, slope[h], slope_col)
    q_in = lax.rem(row, BLOCK)
    col = lax.broadcasted_iota(jnp.int32, (1, picked), 1)
    rows_of = []
    for g in range(nb):
        base = jnp.zeros((1, picked), jnp.int32)
        here = []
        for j in range(topk):
            c = choice[g, j]
            base = jnp.where(col // BLOCK == j, jnp.where(c < 0, NEVER, c * BLOCK), base)
            safe = jnp.where(c < 0, me * nb, c)
            own = safe // nb
            k = me - own
            loc = safe - own * nb
            exact = k == 0
            if n_kv <= 16:
                exact = exact | (k >= FULL_FROM)
            here.append(k * nb + jnp.where(exact, loc, 0))
        rows_of.append(here)
        key_pos = base + lax.rem(col, BLOCK)
        dist = ((me * nb + g) * BLOCK + q_in) - key_pos
        bias[g] = jnp.where(dist >= 0, -slope_col * dist.astype(jnp.float32), -jnp.inf)

    def kv_arrived(k):
        @pl.when(me - k >= 0)
        def _():
            kv_copy(k).wait_recv()

    each(1, n_kv, kv_arrived)

    keep_hi = jnp.where(low, 0.0, 1.0).astype(jnp.bfloat16)
    ones_lo = jnp.where(low, 1.0, 0.0).astype(jnp.bfloat16)

    partner = mt + 1 - 2 * lax.rem(mt, 2)
    peers = [partner]
    for i in range(2, n_tp, 2):
        peers += [lax.rem(mt + i, n_tp), lax.rem(partner + i, n_tp)]

    def att_copy(p, g, source):
        piece = att.at[source, pl.ds(g * BLOCK, BLOCK)]
        return pltpu.make_async_remote_copy(
            src_ref=piece, dst_ref=piece,
            send_sem=att_send.at[p, g], recv_sem=att_recv.at[source, g],
            device_id={"tp": peers[p]})

    def attend(g):
        chosen = jnp.concatenate([table[r] for r in rows_of[g]], axis=0)
        scores = lax.dot_general(q_pad[g], chosen, (((1,), (1,)), ((), ())),
                                 preferred_element_type=jnp.float32) + bias[g]
        top = jnp.max(scores, axis=1, keepdims=True)
        weights = jnp.exp(scores - top).astype(jnp.bfloat16)
        got = jnp.dot(weights, chosen * keep_hi + ones_lo, preferred_element_type=jnp.float32)
        turned = pltpu.roll(got, HEAD, 1)
        parts = []
        for pair in range(heads // 2):
            even = slice(2 * pair * BLOCK, (2 * pair + 1) * BLOCK)
            odd = slice((2 * pair + 1) * BLOCK, (2 * pair + 2) * BLOCK)
            num = jnp.where(low, turned[even], got[odd])
            den = jnp.where(low, got[even], turned[odd])
            parts.append((num / den).astype(jnp.bfloat16))
        return jnp.concatenate(parts, axis=1)

    for first in range(0, nb, GROUP):
        group = range(first, min(first + GROUP, nb))
        done = [attend(g) for g in group]
        for g, value in zip(group, done):
            att[mt, pl.ds(g * BLOCK, BLOCK), :] = value
        for g in group:
            for p in reversed(range(n_tp - 1)):
                att_copy(p, g, mt).start()

    width = heads * HEAD

    def term(source):
        return jnp.dot(att[source], wo[pl.ds(source * width, width)],
                       preferred_element_type=jnp.float32)

    loads[4].wait()
    total = term(mt)
    for p in range(n_tp - 1):
        for g in range(nb):
            att_copy(p, g, peers[p]).wait_recv()
        total += term(peers[p])
    out[...] = total.astype(out.dtype)

    def finish(k):
        if wanted_only(k):
            @pl.when(me - k >= 0)
            def _():
                want_copy(k).wait_send()

        @pl.when(me + k < n_kv)
        def _():
            kv_copy(k).wait_send()

    each(1, n_kv, finish)
    for p in range(n_tp - 1):
        for g in range(nb):
            att_copy(p, g, mt).wait_send()


def shards(n_kv, n_tp, tokens, query_weight, key_weight, value_weight, out_weight, alibi_slope, block_choice):
    rows, depth = tokens.shape
    nb = rows // BLOCK
    width = query_weight.shape[1]
    heads = width // HEAD
    topk = block_choice.shape[1]
    hbm = pl.BlockSpec(memory_space=pltpu.HBM)
    vmem = pl.BlockSpec(memory_space=pltpu.VMEM)
    bf16 = jnp.bfloat16
    dma = pltpu.SemaphoreType.DMA
    return pl.pallas_call(
        functools.partial(kernel, n_kv, n_tp),
        out_shape=pltpu.VMEM((rows, out_weight.shape[1]), bf16),
        in_specs=[hbm] * 7,
        out_specs=vmem,
        scratch_shapes=[
            pltpu.SMEM(alibi_slope.shape, jnp.float32),
            pltpu.SMEM(block_choice.shape, jnp.int32),
            pltpu.VMEM(block_choice.shape, jnp.int32),
            pltpu.VMEM((rows, depth), bf16),
            pltpu.VMEM((depth, width), bf16),
            pltpu.VMEM((LANES, depth), bf16),
            pltpu.VMEM(out_weight.shape, bf16),
            pltpu.VMEM((n_kv * nb, BLOCK, LANES), bf16),
            pltpu.VMEM((n_kv, 8, LANES), jnp.float32),
            pltpu.VMEM((n_kv, 8, LANES), jnp.float32),
            pltpu.VMEM((n_kv, BLOCK, LANES), bf16),
            pltpu.VMEM((nb, heads * BLOCK, LANES), bf16),
            pltpu.VMEM((nb, heads * BLOCK, topk * BLOCK), jnp.float32),
            pltpu.VMEM((n_tp, rows, width), bf16),
            dma((8,)),
            dma((n_kv,)),
            dma((n_kv,)),
            dma((n_kv,)),
            dma((n_kv,)),
            dma((n_tp - 1, nb)),
            dma((n_tp, nb)),
        ],
        compiler_params=pltpu.CompilerParams(collective_id=0, has_side_effects=True),
    )(tokens, query_weight, key_weight.T, value_weight.T, out_weight, alibi_slope, block_choice)


def solution(mesh):
    in_specs = (
        P("kv", None),
        P(None, "tp"),
        P(None, "tp"),
        P(None, "tp"),
        P(None, "tp"),
        P("tp"),
        P("kv", None),
    )
    body = functools.partial(shards, mesh.shape["kv"], mesh.shape["tp"])
    return jax.shard_map(body, mesh=mesh, in_specs=in_specs, out_specs=P("kv", "tp"), check_vma=False)
```

```python
import functools

import jax
import jax.numpy as jnp
from jax import lax
from jax.experimental import pallas as pl
from jax.experimental.pallas import tpu as pltpu
from jax.sharding import PartitionSpec as P

HEAD = 64
BLOCK = 32
LANES = 2 * HEAD
NEVER = 1 << 28
RELAY = 0
FAR = 3
SMALL = 16
GROUP = 2


def each(low, high, body):
    if high - low <= 16:
        for i in range(low, high):
            body(i)
    else:
        pl.loop(low, high)(body)


def when(*conditions):
    if any(c is False for c in conditions):
        return lambda body: None
    return pl.when(functools.reduce(jnp.logical_and, [c for c in conditions if c is not True]))


def negate(condition):
    return not condition if isinstance(condition, bool) else jnp.logical_not(condition)


def kernel(n_kv, n_tp, tok_hbm, wq_hbm, wk_hbm, wv_hbm, wo_hbm, slope_hbm, choice_hbm,
           out, slope, choice, choice_vec, tok, wq, wkv, wo, table, want_out, want_in, send_buf, q_pad, bias, att,
           load_sem, want_send, want_recv, kv_send, kv_recv, att_send, att_recv, fwd_send):
    me = lax.axis_index("kv")
    mt = lax.axis_index("tp")
    rows = tok.shape[0]
    nb = rows // BLOCK
    heads = wq.shape[1] // HEAD
    topk = choice.shape[1]
    picked = topk * BLOCK
    stacked = heads * BLOCK

    loads = [
        pltpu.make_async_copy(tok_hbm, tok, load_sem.at[0]),
        pltpu.make_async_copy(wk_hbm, wkv.at[pl.ds(0, HEAD)], load_sem.at[1]),
        pltpu.make_async_copy(wv_hbm, wkv.at[pl.ds(HEAD, HEAD)], load_sem.at[2]),
        pltpu.make_async_copy(wq_hbm, wq, load_sem.at[3]),
        pltpu.make_async_copy(wo_hbm, wo, load_sem.at[4]),
    ]
    small = [
        pltpu.make_async_copy(choice_hbm, choice_vec, load_sem.at[5]),
        pltpu.make_async_copy(choice_hbm, choice, load_sem.at[6]),
        pltpu.make_async_copy(slope_hbm, slope, load_sem.at[7]),
    ]
    barrier = pltpu.get_barrier_semaphore()

    def far(k, owner):
        if n_kv > SMALL or (k + 1) // 2 < FAR:
            return False
        return True if k // 2 >= FAR else lax.rem(owner, 2) == 1

    def greet(k):
        @pl.when(me + k < n_kv)
        def _():
            pl.semaphore_signal(barrier, inc=1, device_id={"kv": lax.rem(me + k, n_kv)})

        @when(far(k, me + k), me - k >= 0)
        def _():
            pl.semaphore_signal(barrier, inc=1, device_id={"kv": lax.rem(me - k + n_kv, n_kv)})

    each(1, n_kv, greet)
    for d in range(1, n_tp):
        pl.semaphore_signal(barrier, inc=1, device_id={"tp": lax.rem(mt + d, n_tp)})
    for load in small + loads:
        load.start()

    small[0].wait()
    ids = choice_vec[...]
    owner = ids // nb
    local = ids - owner * nb

    def note_want(k):
        hit = (ids >= 0) & (owner == me - k)
        found = jnp.max(jnp.where(hit, local, -1).astype(jnp.float32), keepdims=True)
        want_out[k] = jnp.broadcast_to(found, (8, LANES))

    each(1, n_kv, note_want)

    def want_copy(k):
        return pltpu.make_async_remote_copy(
            src_ref=want_out.at[k], dst_ref=want_in.at[k],
            send_sem=want_send.at[k], recv_sem=want_recv.at[k],
            device_id={"kv": lax.rem(me - k + n_kv, n_kv)})

    def kv_copy(k, unasked=False):
        return pltpu.make_async_remote_copy(
            src_ref=table.at[pl.ds(0, nb)] if unasked else send_buf.at[k],
            dst_ref=table.at[pl.ds(k * nb, nb)] if unasked else table.at[k * nb],
            send_sem=kv_send.at[k], recv_sem=kv_recv.at[k],
            device_id={"kv": lax.rem(me + k, n_kv)})

    def ask(k):
        @when(negate(far(k, me + k)), me - k >= 0)
        def _():
            want_copy(k).start()

    far_peers = 0
    if n_kv <= SMALL:
        for k in range(1, n_kv):
            mine = far(k, me)
            if mine is not False:
                mine = (me + k < n_kv) if mine is True else mine & (me + k < n_kv)
                far_peers += jnp.where(mine, 1, 0)

    def meet():
        pl.semaphore_wait(barrier, me + far_peers + n_tp - 1)
        each(1, n_kv, ask)

    early = far_peers == 0
    if n_kv <= SMALL:
        pl.when(early)(meet)
    else:
        meet()

    for load in loads[:3]:
        load.wait()
    kv = lax.dot_general(tok[...], wkv[...], (((1,), (1,)), ((), ())),
                         preferred_element_type=jnp.float32).astype(jnp.bfloat16)
    table[pl.ds(0, nb)] = kv.reshape(nb, BLOCK, LANES)

    lane = lax.broadcasted_iota(jnp.int32, (1, LANES), 1)
    low = lane < HEAD
    loads[3].wait()
    queries = jnp.dot(tok[...], wq[...], preferred_element_type=jnp.float32)
    queries = queries * (HEAD ** -0.5)
    for pair in range(heads // 2):
        two = queries[:, pair * LANES:(pair + 1) * LANES]
        swapped = pltpu.roll(two, HEAD, 1)
        for half, part in enumerate((two, swapped)):
            part = jnp.where(low, part, 0.0).astype(jnp.bfloat16)
            head = 2 * pair + half
            for g in range(nb):
                q_pad[g, head * BLOCK:(head + 1) * BLOCK, :] = part[g * BLOCK:(g + 1) * BLOCK]

    if n_kv <= SMALL:
        pl.when(jnp.logical_not(early))(meet)

    def send_all(k):
        @when(far(k, me), me + k < n_kv)
        def _():
            kv_copy(k, True).start()

    each(1, n_kv, send_all)

    def answer(k):
        @when(negate(far(k, me)), me + k < n_kv)
        def _():
            want_copy(k).wait_recv()
            want = want_in[k]
            chosen = jnp.zeros((BLOCK // 8, 8, LANES), jnp.float32)
            for b in range(nb):
                blk = table[b].astype(jnp.float32).reshape(BLOCK // 8, 8, LANES)
                chosen = jnp.where((want == float(b))[None], blk, chosen)
            send_buf[k] = chosen.reshape(BLOCK, LANES).astype(jnp.bfloat16)
            kv_copy(k).start()

    each(1, n_kv, answer)

    small[1].wait()
    small[2].wait()
    row = lax.broadcasted_iota(jnp.int32, (stacked, 1), 0)
    slope_col = jnp.zeros((stacked, 1), jnp.float32)
    for h in range(heads):
        slope_col = jnp.where(row // BLOCK == h, slope[h], slope_col)
    q_in = lax.rem(row, BLOCK)
    col = lax.broadcasted_iota(jnp.int32, (1, picked), 1)
    rows_of = []
    for g in range(nb):
        base = jnp.zeros((1, picked), jnp.int32)
        here = []
        for j in range(topk):
            c = choice[g, j]
            base = jnp.where(col // BLOCK == j, jnp.where(c < 0, NEVER, c * BLOCK), base)
            safe = jnp.where(c < 0, me * nb, c)
            own = safe // nb
            k = me - own
            loc = safe - own * nb
            exact = k == 0
            if n_kv <= SMALL:
                exact = exact | (me // 2 - own // 2 >= FAR)
            here.append(k * nb + jnp.where(exact, loc, 0))
        rows_of.append(here)
        key_pos = base + lax.rem(col, BLOCK)
        dist = ((me * nb + g) * BLOCK + q_in) - key_pos
        bias[g] = jnp.where(dist >= 0, -slope_col * dist.astype(jnp.float32), -jnp.inf)

    def kv_arrived(k):
        for unasked in (False, True):
            kind = far(k, me + k)

            @when(kind if unasked else negate(kind), me - k >= 0)
            def _():
                kv_copy(k, unasked).wait_recv()

    each(1, n_kv, kv_arrived)

    keep_hi = jnp.where(low, 0.0, 1.0).astype(jnp.bfloat16)
    ones_lo = jnp.where(low, 1.0, 0.0).astype(jnp.bfloat16)

    partner = mt + 1 - 2 * lax.rem(mt, 2)
    peers = [partner]
    for i in range(2, n_tp, 2):
        peers += [lax.rem(mt + i, n_tp), lax.rem(partner + i, n_tp)]

    def att_copy(p, g, source):
        piece = att.at[source, pl.ds(g * BLOCK, BLOCK)]
        return pltpu.make_async_remote_copy(
            src_ref=piece, dst_ref=piece,
            send_sem=att_send.at[p, g], recv_sem=att_recv.at[source, g],
            device_id={"tp": peers[p]})

    def relayed(p, g):
        return p >= 2 and p % 2 == 0 and g < RELAY

    def forward(p, g):
        piece = att.at[peers[p], pl.ds(g * BLOCK, BLOCK)]
        return pltpu.make_async_remote_copy(
            src_ref=piece, dst_ref=piece,
            send_sem=fwd_send.at[p, g], recv_sem=att_recv.at[peers[p], g],
            device_id={"tp": partner})

    def attend(g):
        chosen = jnp.concatenate([table[r] for r in rows_of[g]], axis=0)
        scores = lax.dot_general(q_pad[g], chosen, (((1,), (1,)), ((), ())),
                                 preferred_element_type=jnp.float32) + bias[g]
        top = jnp.max(scores, axis=1, keepdims=True)
        weights = jnp.exp(scores - top).astype(jnp.bfloat16)
        got = jnp.dot(weights, chosen * keep_hi + ones_lo, preferred_element_type=jnp.float32)
        turned = pltpu.roll(got, HEAD, 1)
        parts = []
        for pair in range(heads // 2):
            even = slice(2 * pair * BLOCK, (2 * pair + 1) * BLOCK)
            odd = slice((2 * pair + 1) * BLOCK, (2 * pair + 2) * BLOCK)
            num = jnp.where(low, turned[even], got[odd])
            den = jnp.where(low, got[even], turned[odd])
            parts.append((num / den).astype(jnp.bfloat16))
        return jnp.concatenate(parts, axis=1)

    for first in range(0, nb, GROUP):
        group = range(first, min(first + GROUP, nb))
        done = [attend(g) for g in group]
        for g, value in zip(group, done):
            att[mt, pl.ds(g * BLOCK, BLOCK), :] = value
        for g in group:
            for p in reversed(range(n_tp - 1)):
                if not relayed(p, g):
                    att_copy(p, g, mt).start()

    width = heads * HEAD

    def term(source):
        return jnp.dot(att[source], wo[pl.ds(source * width, width)],
                       preferred_element_type=jnp.float32)

    loads[4].wait()
    total = term(mt)
    for g in range(min(RELAY, nb)):
        for p in range(1, n_tp - 1, 2):
            att_copy(p, g, peers[p]).wait_recv()
            forward(p, g).start()
    for p in range(n_tp - 1):
        for g in range(nb):
            if not (p % 2 == 1 and g < RELAY):
                att_copy(p, g, peers[p]).wait_recv()
        total += term(peers[p])
    out[...] = total.astype(out.dtype)

    def finish(k):
        @when(negate(far(k, me + k)), me - k >= 0)
        def _():
            want_copy(k).wait_send()

        for unasked in (False, True):
            kind = far(k, me)

            @when(kind if unasked else negate(kind), me + k < n_kv)
            def _():
                kv_copy(k, unasked).wait_send()

    each(1, n_kv, finish)
    for p in range(n_tp - 1):
        for g in range(nb):
            if not relayed(p, g):
                att_copy(p, g, mt).wait_send()
            if p % 2 == 1 and g < RELAY:
                forward(p, g).wait_send()


def shards(n_kv, n_tp, tokens, query_weight, key_weight, value_weight, out_weight, alibi_slope, block_choice):
    rows, depth = tokens.shape
    nb = rows // BLOCK
    width = query_weight.shape[1]
    heads = width // HEAD
    topk = block_choice.shape[1]
    hbm = pl.BlockSpec(memory_space=pltpu.HBM)
    vmem = pl.BlockSpec(memory_space=pltpu.VMEM)
    bf16 = jnp.bfloat16
    dma = pltpu.SemaphoreType.DMA
    return pl.pallas_call(
        functools.partial(kernel, n_kv, n_tp),
        out_shape=pltpu.VMEM((rows, out_weight.shape[1]), bf16),
        in_specs=[hbm] * 7,
        out_specs=vmem,
        scratch_shapes=[
            pltpu.SMEM(alibi_slope.shape, jnp.float32),
            pltpu.SMEM(block_choice.shape, jnp.int32),
            pltpu.VMEM(block_choice.shape, jnp.int32),
            pltpu.VMEM((rows, depth), bf16),
            pltpu.VMEM((depth, width), bf16),
            pltpu.VMEM((LANES, depth), bf16),
            pltpu.VMEM(out_weight.shape, bf16),
            pltpu.VMEM((n_kv * nb, BLOCK, LANES), bf16),
            pltpu.VMEM((n_kv, 8, LANES), jnp.float32),
            pltpu.VMEM((n_kv, 8, LANES), jnp.float32),
            pltpu.VMEM((n_kv, BLOCK, LANES), bf16),
            pltpu.VMEM((nb, heads * BLOCK, LANES), bf16),
            pltpu.VMEM((nb, heads * BLOCK, topk * BLOCK), jnp.float32),
            pltpu.VMEM((n_tp, rows, width), bf16),
            dma((8,)),
            dma((n_kv,)),
            dma((n_kv,)),
            dma((n_kv,)),
            dma((n_kv,)),
            dma((n_tp - 1, nb)),
            dma((n_tp, nb)),
            dma((n_tp - 1, nb)),
        ],
        compiler_params=pltpu.CompilerParams(collective_id=0, has_side_effects=True),
    )(tokens, query_weight, key_weight.T, value_weight.T, out_weight, alibi_slope, block_choice)


def solution(mesh):
    in_specs = (
        P("kv", None),
        P(None, "tp"),
        P(None, "tp"),
        P(None, "tp"),
        P(None, "tp"),
        P("tp"),
        P("kv", None),
    )
    body = functools.partial(shards, mesh.shape["kv"], mesh.shape["tp"])
    return jax.shard_map(body, mesh=mesh, in_specs=in_specs, out_specs=P("kv", "tp"), check_vma=False)
```

```python
import functools

import jax
import jax.numpy as jnp
from jax import lax
from jax.experimental import pallas as pl
from jax.experimental.pallas import tpu as pltpu
from jax.sharding import PartitionSpec as P

HEAD = 64
BLOCK = 32
LANES = 2 * HEAD
NEVER = 1 << 28
RELAY = 0
FAR = 3
SMALL = 16
GROUP = 2


def each(low, high, body):
    if high - low <= 16:
        for i in range(low, high):
            body(i)
    else:
        pl.loop(low, high)(body)


def when(*conditions):
    if any(c is False for c in conditions):
        return lambda body: None
    return pl.when(functools.reduce(jnp.logical_and, [c for c in conditions if c is not True]))


def negate(condition):
    return not condition if isinstance(condition, bool) else jnp.logical_not(condition)


def kernel(n_kv, n_tp, tok_hbm, wq_hbm, wk_hbm, wv_hbm, wo_hbm, slope_hbm, choice_hbm,
           out, slope, choice, choice_vec, tok, wq, wkv, wo, table, want_out, want_in, send_buf, q_pad, bias, att,
           load_sem, want_send, want_recv, kv_send, kv_recv, att_send, att_recv, fwd_send):
    me = lax.axis_index("kv")
    mt = lax.axis_index("tp")
    rows = tok.shape[0]
    nb = rows // BLOCK
    heads = wq.shape[1] // HEAD
    topk = choice.shape[1]
    step = GROUP if nb % GROUP == 0 else 1
    pieces = nb // step
    picked = topk * BLOCK
    stacked = heads * BLOCK

    loads = [
        pltpu.make_async_copy(tok_hbm, tok, load_sem.at[0]),
        pltpu.make_async_copy(wk_hbm, wkv.at[pl.ds(0, HEAD)], load_sem.at[1]),
        pltpu.make_async_copy(wv_hbm, wkv.at[pl.ds(HEAD, HEAD)], load_sem.at[2]),
        pltpu.make_async_copy(wq_hbm, wq, load_sem.at[3]),
        pltpu.make_async_copy(wo_hbm, wo, load_sem.at[4]),
    ]
    small = [
        pltpu.make_async_copy(choice_hbm, choice_vec, load_sem.at[5]),
        pltpu.make_async_copy(choice_hbm, choice, load_sem.at[6]),
        pltpu.make_async_copy(slope_hbm, slope, load_sem.at[7]),
    ]
    barrier = pltpu.get_barrier_semaphore()

    def far(k, owner):
        if n_kv > SMALL or (k + 1) // 2 < FAR:
            return False
        return True if k // 2 >= FAR else lax.rem(owner, 2) == 1

    def greet(k):
        @pl.when(me + k < n_kv)
        def _():
            pl.semaphore_signal(barrier, inc=1, device_id={"kv": lax.rem(me + k, n_kv)})

        @when(far(k, me + k), me - k >= 0)
        def _():
            pl.semaphore_signal(barrier, inc=1, device_id={"kv": lax.rem(me - k + n_kv, n_kv)})

    each(1, n_kv, greet)
    for d in range(1, n_tp):
        pl.semaphore_signal(barrier, inc=1, device_id={"tp": lax.rem(mt + d, n_tp)})
    for load in small + loads:
        load.start()

    small[0].wait()
    ids = choice_vec[...]
    owner = ids // nb
    local = ids - owner * nb

    def note_want(k):
        hit = (ids >= 0) & (owner == me - k)
        found = jnp.max(jnp.where(hit, local, -1).astype(jnp.float32), keepdims=True)
        want_out[k] = jnp.broadcast_to(found, (8, LANES))

    each(1, n_kv, note_want)

    def want_copy(k):
        return pltpu.make_async_remote_copy(
            src_ref=want_out.at[k], dst_ref=want_in.at[k],
            send_sem=want_send.at[k], recv_sem=want_recv.at[k],
            device_id={"kv": lax.rem(me - k + n_kv, n_kv)})

    def kv_copy(k, unasked=False):
        return pltpu.make_async_remote_copy(
            src_ref=table.at[pl.ds(0, nb)] if unasked else send_buf.at[k],
            dst_ref=table.at[pl.ds(k * nb, nb)] if unasked else table.at[k * nb],
            send_sem=kv_send.at[k], recv_sem=kv_recv.at[k],
            device_id={"kv": lax.rem(me + k, n_kv)})

    def ask(k):
        @when(negate(far(k, me + k)), me - k >= 0)
        def _():
            want_copy(k).start()

    far_peers = 0
    if n_kv <= SMALL:
        for k in range(1, n_kv):
            mine = far(k, me)
            if mine is not False:
                mine = (me + k < n_kv) if mine is True else mine & (me + k < n_kv)
                far_peers += jnp.where(mine, 1, 0)

    def meet():
        pl.semaphore_wait(barrier, me + far_peers + n_tp - 1)
        each(1, n_kv, ask)

    early = far_peers == 0
    if n_kv <= SMALL:
        pl.when(early)(meet)
    else:
        meet()

    for load in loads[:3]:
        load.wait()
    kv = lax.dot_general(tok[...], wkv[...], (((1,), (1,)), ((), ())),
                         preferred_element_type=jnp.float32).astype(jnp.bfloat16)
    table[pl.ds(0, nb)] = kv.reshape(nb, BLOCK, LANES)

    lane = lax.broadcasted_iota(jnp.int32, (1, LANES), 1)
    low = lane < HEAD
    loads[3].wait()
    queries = jnp.dot(tok[...], wq[...], preferred_element_type=jnp.float32)
    queries = queries * (HEAD ** -0.5)
    for pair in range(heads // 2):
        two = queries[:, pair * LANES:(pair + 1) * LANES]
        swapped = pltpu.roll(two, HEAD, 1)
        for half, part in enumerate((two, swapped)):
            part = jnp.where(low, part, 0.0).astype(jnp.bfloat16)
            head = 2 * pair + half
            for g in range(nb):
                q_pad[g, head * BLOCK:(head + 1) * BLOCK, :] = part[g * BLOCK:(g + 1) * BLOCK]

    if n_kv <= SMALL:
        pl.when(jnp.logical_not(early))(meet)

    def send_all(k):
        @when(far(k, me), me + k < n_kv)
        def _():
            kv_copy(k, True).start()

    each(1, n_kv, send_all)

    def answer(k):
        @when(negate(far(k, me)), me + k < n_kv)
        def _():
            want_copy(k).wait_recv()
            want = want_in[k]
            chosen = jnp.zeros((BLOCK // 8, 8, LANES), jnp.float32)
            for b in range(nb):
                blk = table[b].astype(jnp.float32).reshape(BLOCK // 8, 8, LANES)
                chosen = jnp.where((want == float(b))[None], blk, chosen)
            send_buf[k] = chosen.reshape(BLOCK, LANES).astype(jnp.bfloat16)
            kv_copy(k).start()

    each(1, n_kv, answer)

    small[1].wait()
    small[2].wait()
    row = lax.broadcasted_iota(jnp.int32, (stacked, 1), 0)
    slope_col = jnp.zeros((stacked, 1), jnp.float32)
    for h in range(heads):
        slope_col = jnp.where(row // BLOCK == h, slope[h], slope_col)
    q_in = lax.rem(row, BLOCK)
    col = lax.broadcasted_iota(jnp.int32, (1, picked), 1)
    rows_of = []
    for g in range(nb):
        base = jnp.zeros((1, picked), jnp.int32)
        here = []
        for j in range(topk):
            c = choice[g, j]
            base = jnp.where(col // BLOCK == j, jnp.where(c < 0, NEVER, c * BLOCK), base)
            safe = jnp.where(c < 0, me * nb, c)
            own = safe // nb
            k = me - own
            loc = safe - own * nb
            exact = k == 0
            if n_kv <= SMALL:
                exact = exact | (me // 2 - own // 2 >= FAR)
            here.append(k * nb + jnp.where(exact, loc, 0))
        rows_of.append(here)
        key_pos = base + lax.rem(col, BLOCK)
        dist = ((me * nb + g) * BLOCK + q_in) - key_pos
        bias[g] = jnp.where(dist >= 0, -slope_col * dist.astype(jnp.float32), -jnp.inf)

    def kv_arrived(k):
        for unasked in (False, True):
            kind = far(k, me + k)

            @when(kind if unasked else negate(kind), me - k >= 0)
            def _():
                kv_copy(k, unasked).wait_recv()

    each(1, n_kv, kv_arrived)

    keep_hi = jnp.where(low, 0.0, 1.0).astype(jnp.bfloat16)
    ones_lo = jnp.where(low, 1.0, 0.0).astype(jnp.bfloat16)

    partner = mt + 1 - 2 * lax.rem(mt, 2)
    peers = [partner]
    for i in range(2, n_tp, 2):
        peers += [lax.rem(mt + i, n_tp), lax.rem(partner + i, n_tp)]

    def att_copy(p, g, source):
        piece = att.at[source, pl.ds(g * step * BLOCK, step * BLOCK)]
        return pltpu.make_async_remote_copy(
            src_ref=piece, dst_ref=piece,
            send_sem=att_send.at[p, g], recv_sem=att_recv.at[source, g],
            device_id={"tp": peers[p]})

    def relayed(p, g):
        return p >= 2 and p % 2 == 0 and g < RELAY

    def forward(p, g):
        piece = att.at[peers[p], pl.ds(g * step * BLOCK, step * BLOCK)]
        return pltpu.make_async_remote_copy(
            src_ref=piece, dst_ref=piece,
            send_sem=fwd_send.at[p, g], recv_sem=att_recv.at[peers[p], g],
            device_id={"tp": partner})

    def attend(g):
        chosen = jnp.concatenate([table[r] for r in rows_of[g]], axis=0)
        scores = lax.dot_general(q_pad[g], chosen, (((1,), (1,)), ((), ())),
                                 preferred_element_type=jnp.float32) + bias[g]
        top = jnp.max(scores, axis=1, keepdims=True)
        weights = jnp.exp(scores - top).astype(jnp.bfloat16)
        got = jnp.dot(weights, chosen * keep_hi + ones_lo, preferred_element_type=jnp.float32)
        turned = pltpu.roll(got, HEAD, 1)
        parts = []
        for pair in range(heads // 2):
            even = slice(2 * pair * BLOCK, (2 * pair + 1) * BLOCK)
            odd = slice((2 * pair + 1) * BLOCK, (2 * pair + 2) * BLOCK)
            num = jnp.where(low, turned[even], got[odd])
            den = jnp.where(low, got[even], turned[odd])
            parts.append((num / den).astype(jnp.bfloat16))
        return jnp.concatenate(parts, axis=1)

    for first in range(0, nb, step):
        group = range(first, first + step)
        done = [attend(g) for g in group]
        for g, value in zip(group, done):
            att[mt, pl.ds(g * BLOCK, BLOCK), :] = value
        for p in reversed(range(n_tp - 1)):
            if not relayed(p, first // step):
                att_copy(p, first // step, mt).start()

    width = heads * HEAD

    def term(source):
        return jnp.dot(att[source], wo[pl.ds(source * width, width)],
                       preferred_element_type=jnp.float32)

    loads[4].wait()
    total = term(mt)
    for g in range(min(RELAY, pieces)):
        for p in range(1, n_tp - 1, 2):
            att_copy(p, g, peers[p]).wait_recv()
            forward(p, g).start()
    span = step * BLOCK
    for g in range(pieces):
        here = slice(g * span, (g + 1) * span)
        part = total[here]
        for p in range(n_tp - 1):
            if not (p % 2 == 1 and g < RELAY):
                att_copy(p, g, peers[p]).wait_recv()
            part += jnp.dot(att[peers[p], here, :], wo[pl.ds(peers[p] * width, width)],
                            preferred_element_type=jnp.float32)
        out[here, :] = part.astype(out.dtype)

    def finish(k):
        @when(negate(far(k, me + k)), me - k >= 0)
        def _():
            want_copy(k).wait_send()

        for unasked in (False, True):
            kind = far(k, me)

            @when(kind if unasked else negate(kind), me + k < n_kv)
            def _():
                kv_copy(k, unasked).wait_send()

    each(1, n_kv, finish)
    for p in range(n_tp - 1):
        for g in range(pieces):
            if not relayed(p, g):
                att_copy(p, g, mt).wait_send()
            if p % 2 == 1 and g < RELAY:
                forward(p, g).wait_send()


def shards(n_kv, n_tp, tokens, query_weight, key_weight, value_weight, out_weight, alibi_slope, block_choice):
    rows, depth = tokens.shape
    nb = rows // BLOCK
    width = query_weight.shape[1]
    heads = width // HEAD
    topk = block_choice.shape[1]
    hbm = pl.BlockSpec(memory_space=pltpu.HBM)
    vmem = pl.BlockSpec(memory_space=pltpu.VMEM)
    bf16 = jnp.bfloat16
    dma = pltpu.SemaphoreType.DMA
    return pl.pallas_call(
        functools.partial(kernel, n_kv, n_tp),
        out_shape=pltpu.VMEM((rows, out_weight.shape[1]), bf16),
        in_specs=[hbm] * 7,
        out_specs=vmem,
        scratch_shapes=[
            pltpu.SMEM(alibi_slope.shape, jnp.float32),
            pltpu.SMEM(block_choice.shape, jnp.int32),
            pltpu.VMEM(block_choice.shape, jnp.int32),
            pltpu.VMEM((rows, depth), bf16),
            pltpu.VMEM((depth, width), bf16),
            pltpu.VMEM((LANES, depth), bf16),
            pltpu.VMEM(out_weight.shape, bf16),
            pltpu.VMEM((n_kv * nb, BLOCK, LANES), bf16),
            pltpu.VMEM((n_kv, 8, LANES), jnp.float32),
            pltpu.VMEM((n_kv, 8, LANES), jnp.float32),
            pltpu.VMEM((n_kv, BLOCK, LANES), bf16),
            pltpu.VMEM((nb, heads * BLOCK, LANES), bf16),
            pltpu.VMEM((nb, heads * BLOCK, topk * BLOCK), jnp.float32),
            pltpu.VMEM((n_tp, rows, width), bf16),
            dma((8,)),
            dma((n_kv,)),
            dma((n_kv,)),
            dma((n_kv,)),
            dma((n_kv,)),
            dma((n_tp - 1, nb)),
            dma((n_tp, nb)),
            dma((n_tp - 1, nb)),
        ],
        compiler_params=pltpu.CompilerParams(collective_id=0, has_side_effects=True),
    )(tokens, query_weight, key_weight.T, value_weight.T, out_weight, alibi_slope, block_choice)


def solution(mesh):
    in_specs = (
        P("kv", None),
        P(None, "tp"),
        P(None, "tp"),
        P(None, "tp"),
        P(None, "tp"),
        P("tp"),
        P("kv", None),
    )
    body = functools.partial(shards, mesh.shape["kv"], mesh.shape["tp"])
    return jax.shard_map(body, mesh=mesh, in_specs=in_specs, out_specs=P("kv", "tp"), check_vma=False)
```
